512 devices in a mesh: grp: 2 (over y), sp: 32 (over z, core), tp: 8 (over x).
Axes of the slice: x: 8, y: 2, z: 16, core: 2. Of those that a mesh axis runs over, the one named last changes fastest.
The devices are a block of a 8x8x16 slice.
Arguments:
- tokens: bfloat16 [8192, 2048], P(('grp', 'sp'), 'tp'), parts along dimension 0, may hold values from -30 to 30, as said below
- norm_gain: float32 [2, 2048], replicated, may hold values from 0.1 to 1.9
- in_weight: bfloat16 [2, 2048, 2048], P(None, 'sp', 'tp'), may hold values from -0.125 to 0.125
- gate_weight: bfloat16 [2, 2048, 2048], P(None, 'sp', 'tp'), may hold values from -0.125 to 0.125
- conv_taps: float32 [2, 4, 2048], P(None, None, 'tp'), may hold values from -3 to 3
- decay_logit: float32 [2, 2, 2048], P(None, None, 'tp'), may hold values from 4 to 20, as said below
- gate_maps: bfloat16 [2, 2048, 1024], P(None, 'tp', 'sp'), may hold values from -0.375 to 0.375
- out_weight: bfloat16 [2, 2048, 2048], P(None, 'sp', 'tp'), may hold values from -0.375 to 0.375
- final_gain: float32 [2048], P('tp'), may hold values from 0.1 to 1.9
Outputs:
- normed_out: bfloat16 [8192, 2048], P(('grp', 'sp'), 'tp'), parts along dimension 0
The draws below stay inside these ranges and needn't reach their ends.
There are 2 independent parts, one for each index of `grp`. The reference program is written for one: setup_inputs(seed, part) draws one part's arguments, and reference() takes and returns one part's arrays. A program takes and returns all parts, laid end to end along the dimension named above; an argument that names none is the same for every part. Nothing has to cross between parts.
Inputs may be any that keep to these rules, and one draw needn't show every extreme that they name: Activations of order one whose scale changes by blocks of tokens and of channels. `decay_logit`: decay parameters; channels differ in how far their state reaches.
All inputs are finite; a program needn't handle non-finite values.
Results may differ from the reference program's by a relative error of at most 0.02.
Values may be sent and summed in bfloat16 or wider, within the bound.
A program may use at most 128 MiB of HBM per device.

```python
import jax
import jax.numpy as jnp
from jax import lax

D = 2048
HEADS = 8
HEAD_W = 256
TAPS = 4
LAYERS = 2
TOK_DEV = 128
WIDTH_R = 2048
TOKENS = 4096


def draw_tokens(key, part):
    first, second, third = jax.random.split(key, 3)
    base = jnp.clip(jax.random.normal(first, (TOKENS, D), jnp.float32), -5.0, 5.0)
    span = TOK_DEV // 2
    row_scale = jnp.exp(jax.random.uniform(second, (TOKENS // span,), jnp.float32, jnp.log(0.4), jnp.log(2.0)))
    col_scale = jnp.exp(jax.random.uniform(third, (8,), jnp.float32, jnp.log(0.35), jnp.log(2.8)))
    rows = jnp.repeat(row_scale, span)
    cols = jnp.repeat(col_scale, D // 8)
    return (base * rows[:, None] * cols[None, :]).astype(jnp.bfloat16)


def draw_decay_logit(key, part):
    first, second, third = jax.random.split(key, 3)
    shape = (LAYERS, 2, WIDTH_R)
    share = 0.5
    quick = jax.random.uniform(first, shape, jnp.float32) < share
    slow_rate = jnp.exp(jax.random.uniform(second, shape, jnp.float32, jnp.log(0.02), jnp.log(0.25))) / TOKENS
    quick_rate = jnp.exp(jax.random.uniform(third, shape, jnp.float32, jnp.log(0.0025), jnp.log(0.0083)))
    rate = jnp.where(quick, quick_rate, slow_rate)
    return -jnp.log(jnp.expm1(rate))


def levels(key, extent, pieces, low, high):
    gain, own = 1.0, jax.random.fold_in(key, 6)
    for axis_at, shards_of in pieces:
        heights = jnp.exp(jax.random.uniform(jax.random.fold_in(own, axis_at), (shards_of,), jnp.float32, low / len(pieces), high / len(pieces)))
        gain = gain * jnp.repeat(heights, extent[axis_at] // shards_of).reshape([-1 if axis == axis_at else 1 for axis in range(len(extent))])
    return gain


def bell_draw(rng, shape, spread, most, shards=(), dtype=jnp.bfloat16):
    level = levels(rng, shape, shards, -0.22, 0.18) if shards else 1.0
    values = jax.random.normal(rng, shape, jnp.float32) * spread * level
    return jnp.minimum(jnp.maximum(values, -most), most).astype(dtype)


def setup_inputs(seed: int = 0, part: int = 0) -> dict:
    key_of = jax.random.split(jax.random.key(seed), 10)
    own_keys = jax.random.split(jax.random.fold_in(key_of[9], part), 10)
    return {
        "tokens": draw_tokens(jax.random.fold_in(jax.random.fold_in(key_of[9], part), 71), part),
        "norm_gain": jnp.clip(1.0 + 0.18 * jax.random.normal(key_of[1], (LAYERS, D), jnp.float32), 0.1, 1.9),
        "in_weight": bell_draw(key_of[2], (LAYERS, D, WIDTH_R), D ** -0.5, 0.125, ((1, 32), (2, 8))),
        "gate_weight": bell_draw(key_of[3], (LAYERS, D, WIDTH_R), D ** -0.5, 0.125, ((1, 32), (2, 8))),
        "conv_taps": bell_draw(key_of[4], (LAYERS, TAPS, WIDTH_R), 0.5, 3.0, ((2, 8),), jnp.float32),
        "decay_logit": draw_decay_logit(jax.random.fold_in(key_of[9], 71), part),
        "gate_maps": bell_draw(key_of[6], (LAYERS, WIDTH_R, 4 * HEAD_W), HEAD_W ** -0.5, 0.375, ((1, 8), (2, 32))),
        "out_weight": bell_draw(key_of[7], (LAYERS, WIDTH_R, D), (WIDTH_R // 8) ** -0.5, 0.375, ((1, 32), (2, 8))),
        "final_gain": jnp.clip(1.0 + 0.18 * jax.random.normal(key_of[8], (D,), jnp.float32), 0.1, 1.9),
    }


EPS = 1e-06

def combine_pair(earlier, later):
    return (earlier[0] * later[0], later[0] * earlier[1] + later[1])

def reference(tokens, norm_gain, in_weight, gate_weight, conv_taps, decay_logit, gate_maps, out_weight, final_gain):
    resid = tokens
    length = tokens.shape[0]
    for layer in range(LAYERS):
        wide = resid.astype(jnp.float32)
        normed = (wide * lax.rsqrt(lax.optimization_barrier(jnp.mean(wide * wide, axis=1, keepdims=True)) + EPS) * norm_gain[layer]).astype(jnp.bfloat16)
        xin = jnp.dot(normed, in_weight[layer], preferred_element_type=jnp.float32).astype(jnp.bfloat16)
        gin = jnp.dot(normed, gate_weight[layer], preferred_element_type=jnp.float32).astype(jnp.bfloat16)
        padded = jnp.pad(xin.astype(jnp.float32), ((2, 1), (0, 0)))
        conv = conv_taps[layer, 0] * padded[0:length]
        for k in range(1, TAPS):
            conv = conv + conv_taps[layer, k] * padded[k:k + length]
        conv = conv.astype(jnp.bfloat16)
        stacked = conv.astype(jnp.float32).reshape(length, HEADS, HEAD_W)
        maps = gate_maps[layer].astype(jnp.float32).reshape(HEADS, HEAD_W, 4 * HEAD_W)
        pre = jnp.einsum('thi,hij->thj', stacked, maps).reshape(length, HEADS, 4, HEAD_W)
        conv32 = conv.astype(jnp.float32)
        states = []
        for direction in range(2):
            rate = jax.nn.sigmoid(pre[:, :, 2 * direction]).reshape(length, WIDTH_R)
            inp = jax.nn.sigmoid(pre[:, :, 2 * direction + 1]).reshape(length, WIDTH_R)
            log_a = -8.0 * rate * jax.nn.softplus(-decay_logit[layer, direction])
            decay = jnp.exp(log_a)
            drive = jnp.sqrt(-jnp.expm1(2.0 * log_a)) * inp * conv32
            _, state = lax.associative_scan(combine_pair, (decay, drive), reverse=direction == 1, axis=0)
            states.append(state)
        mix = (jax.nn.gelu(gin.astype(jnp.float32)) * (states[0] + states[1])).astype(jnp.bfloat16)
        out = jnp.dot(mix, out_weight[layer], preferred_element_type=jnp.float32)
        resid = (resid.astype(jnp.float32) + out).astype(jnp.bfloat16)
    wide = resid.astype(jnp.float32)
    return (wide * lax.rsqrt(lax.optimization_barrier(jnp.mean(wide * wide, axis=1, keepdims=True)) + EPS) * final_gain).astype(jnp.bfloat16)
```

```python
import functools

import jax
import jax.numpy as jnp
from jax import lax
from jax.experimental import pallas as pl
from jax.experimental.pallas import tpu as pltpu
from jax.sharding import PartitionSpec as P

HEAD_W = 256
TAPS = 4
LAYERS = 2
EPS = 1e-06
F32 = jnp.float32
BF16 = jnp.bfloat16


def remote(src, dst, send, recv, where):
    return pltpu.make_async_remote_copy(
        src_ref=src,
        dst_ref=dst,
        send_sem=send,
        recv_sem=recv,
        device_id=where,
        device_id_type=pl.DeviceIdType.MESH,
    )


def bytes_of(ref, sem):
    return pltpu.make_async_copy(ref, ref, sem)


def softplus_small(x):
    y = jnp.exp(-jnp.abs(x))
    series = y * (1 - y * (1 / 2 - y * (1 / 3 - y * (1 / 4 - y * (1 / 5 - y * (1 / 6))))))
    return jnp.maximum(x, 0.0) + jnp.where(y < 0.05, series, jnp.log(1.0 + y))


def neg_expm1(x):
    tail = 1 + x * (1 / 6) * (1 + x * (1 / 7) * (1 + x * (1 / 8)))
    series = x * (1 + x * (1 / 2) * (1 + x * (1 / 3) * (1 + x * (1 / 4) * (1 + x * (1 / 5) * tail))))
    return -jnp.where(x > -0.5, series, jnp.exp(x) - 1.0)


class Ring:
    def __init__(self, held, sems, size, place):
        self.held, self.place, self.size = held, place, size
        self.send, self.recv, self.push_send, self.push_recv = sems
        self.chips = size // 2
        self.half = self.chips // 2
        self.chip, self.core = place // 2, lax.rem(place, 2)
        self.rows = held.shape[1]

    def slot(self, chip):
        return lax.rem(chip + 2 * self.chips, self.chips) * 2 + self.core

    def view(self, slot, flow, step):
        if step < self.half:
            return self.held.at[slot]
        rows = self.rows // 2
        return self.held.at[slot, pl.ds(flow * rows, rows)]

    def hop(self, flow, step):
        way = 1 - 2 * flow
        view = self.view(self.slot(self.chip - way * (step - 1)), flow, step)
        return remote(
            view, view, self.send, self.recv.at[flow, step - 1], {"sp": self.slot(self.chip + way)}
        )

    def landed(self, flow, step):
        way = 1 - 2 * flow
        view = self.view(self.slot(self.chip - way * step), flow, step)
        return remote(
            view, view, self.send, self.recv.at[flow, step - 1], {"sp": self.slot(self.chip + way)}
        )

    def push(self, slot):
        view = self.held.at[slot]
        other = self.chip * 2 + 1 - self.core
        remote(view, view, self.push_send, self.push_recv, {"sp": other}).start()

    def begin(self):
        for flow in range(2):
            self.hop(flow, 1).start()
        self.push(self.place)

    def step(self, step):
        for flow in range(2):
            self.landed(flow, step).wait_recv()
            if step < self.half:
                self.hop(flow, step + 1).start()
                way = 1 - 2 * flow
                self.push(self.slot(self.chip - way * step))
        if step == self.half:
            self.push(self.slot(self.chip + self.half))

    def joined(self):
        bytes_of(self.held.at[pl.ds(0, self.chips)], self.push_recv).wait()

    def drain(self):
        bytes_of(self.held.at[pl.ds(0, self.chips - 1)], self.send).wait()
        bytes_of(self.held.at[pl.ds(0, self.chips)], self.push_send).wait()


class Spread:
    def __init__(self, held, send, recv, size, place):
        self.held, self.send, self.recv = held, send, recv
        self.size, self.place = size, place
        self.order = sorted(range(1, size), key=lambda d: -min(d, size - d))

    def begin(self, block):
        for d in self.order:
            peer = lax.rem(self.place + d, self.size)
            remote(
                block, self.held.at[self.place], self.send, self.recv.at[d - 1], {"tp": peer}
            ).start()

    def wait(self):
        for d in self.order:
            slot = self.held.at[lax.rem(self.place + self.size - d, self.size)]
            remote(slot, slot, self.send, self.recv.at[d - 1], {"tp": self.place}).wait_recv()

    def drain(self):
        bytes_of(self.held.at[pl.ds(0, self.size - 1)], self.send).wait()


def kernel(
    S,
    T,
    tokens,
    norm_gain,
    in_weight,
    gate_weight,
    conv_taps,
    decay_logit,
    gate_maps,
    out_weight,
    final_gain,
    out,
    held_a,
    held_b,
    held_c,
    acts,
    edges,
    edge_in,
    padded,
    coef,
    local,
    hidden,
    gated,
    msg,
    carries,
    block,
    squares,
    ring_recv,
    ring_send,
    x_recv,
    x_send,
    edge_sems,
    carry_sems,
    square_sems,
):
    p = lax.axis_index("sp")
    t = lax.axis_index("tp")
    rows, width = tokens.shape
    depth = in_weight.shape[1]
    cols = gate_maps.shape[2]
    seg = rows // 8
    share = width // depth
    quarter = S // 4

    barrier = pltpu.get_barrier_semaphore()
    for d in range(1, T):
        pl.semaphore_signal(
            barrier, inc=1, device_id={"tp": lax.rem(t + d, T)}, device_id_type=pl.DeviceIdType.MESH
        )
    for d in range(1, S):
        pl.semaphore_signal(
            barrier, inc=1, device_id={"sp": lax.rem(p + d, S)}, device_id_type=pl.DeviceIdType.MESH
        )

    eye = (
        lax.broadcasted_iota(jnp.int32, (cols, cols), 0)
        == lax.broadcasted_iota(jnp.int32, (cols, cols), 1)
    ).astype(BF16)

    def turned(layer):
        return lax.dot_general(
            eye, gate_maps[layer], (((1,), (1,)), ((), ())), preferred_element_type=F32
        ).astype(BF16)

    held_a[p, 0:depth] = in_weight[0]
    held_a[p, depth : depth + cols] = turned(0)
    held_b[p, 0:depth] = gate_weight[0]
    held_b[p, depth : 2 * depth] = out_weight[0]
    held_c[p, 0:depth] = in_weight[1]
    held_c[p, depth : depth + cols] = turned(1)
    held_c[p, depth + cols : 2 * depth + cols] = gate_weight[1]
    held_c[p, 2 * depth + cols : 3 * depth + cols] = out_weight[1]
    acts[0, t] = tokens[...]

    pl.semaphore_wait(barrier, T + S - 2)

    def ring(held, k):
        return Ring(
            held,
            (ring_send.at[k, 0], ring_recv.at[k], ring_send.at[k, 1], ring_send.at[k, 2]),
            S,
            p,
        )

    ring_a, ring_b, ring_c = ring(held_a, 0), ring(held_b, 1), ring(held_c, 2)
    spread = [Spread(acts.at[k], x_send.at[k], x_recv.at[k], T, t) for k in range(4)]

    ring_a.begin()
    spread[0].begin(tokens)
    ring_b.begin()
    for step in range(1, S // 4 + 1):
        ring_a.step(step)
        ring_b.step(step)
    ring_c.begin()
    spread[0].wait()
    ring_a.joined()

    later = iter(range(1, S // 4 + 1))

    def forward_some():
        step = next(later, None)
        if step is not None:
            ring_c.step(step)

    for layer in range(LAYERS):
        if layer == 0:
            in_at, map_at, gate_at, out_at = (held_a, 0), (held_a, depth), (held_b, 0), (held_b, depth)
        else:
            for _ in range(S // 4):
                forward_some()
            ring_c.joined()
            in_at, map_at = (held_c, 0), (held_c, depth)
            gate_at, out_at = (held_c, depth + cols), (held_c, 2 * depth + cols)

        def weight(at, k):
            held, row = at
            return held[k * share : (k + 1) * share, row : row + depth].reshape(width, width)

        full = acts.at[2 * layer]
        total = jnp.zeros((rows, 1), F32)
        for k in range(T):
            wide = full[k].astype(F32)
            total = total + jnp.sum(wide * wide, axis=1, keepdims=True)
        scale = lax.rsqrt(total / (T * width) + EPS)
        proj = jnp.zeros((rows, width), F32)
        for k in range(T):
            wide = full[k].astype(F32)
            normed = (
                wide * scale * norm_gain[layer : layer + 1, k * width : (k + 1) * width]
            ).astype(BF16)
            full[k] = normed
            proj = proj + jnp.dot(normed, weight(in_at, k), preferred_element_type=F32)
        xin = proj.astype(BF16)
        edges[layer, 0] = xin[rows - 16 : rows]
        edges[layer, 1] = xin[0:16]
        up = remote(
            edges.at[layer, 0], edge_in.at[layer, 0], edge_sems.at[layer, 0], edge_sems.at[layer, 1],
            {"sp": lax.rem(p + 1, S)},
        )
        down = remote(
            edges.at[layer, 1], edge_in.at[layer, 1], edge_sems.at[layer, 2], edge_sems.at[layer, 3],
            {"sp": lax.rem(p + S - 1, S)},
        )
        up.start()
        down.start()
        padded[8 : 8 + rows] = xin.astype(F32)
        if layer == 0:
            ring_b.joined()
        forward_some()
        proj = jnp.zeros((rows, width), F32)
        for k in range(T):
            proj = proj + jnp.dot(full[k], weight(gate_at, k), preferred_element_type=F32)
        gated[...] = jax.nn.gelu(proj.astype(BF16).astype(F32))
        up.wait()
        down.wait()
        forward_some()
        before = edge_in[layer, 0].astype(F32)[8:16]
        after = edge_in[layer, 1].astype(F32)[0:8]
        padded[0:8] = jnp.where(p == 0, 0.0, before)
        padded[8 + rows : 16 + rows] = jnp.where(p == S - 1, 0.0, after)
        conv = conv_taps[layer, 0:1] * padded[6 : 6 + rows]
        for k in range(1, TAPS):
            conv = conv + conv_taps[layer, k : k + 1] * padded[6 + k : 6 + k + rows]
        conv = conv.astype(BF16)
        conv32 = conv.astype(F32)

        def gate(g):
            held, row = map_at
            maps = held[g * quarter : (g + 1) * quarter, row : row + cols].reshape(width, width)
            pre = lax.dot_general(
                conv, maps, (((1,), (1,)), ((), ())), preferred_element_type=F32
            )
            return jax.nn.sigmoid(pre)

        first = []
        for way in range(2):
            log_a = (
                -8.0 * gate(2 * way) * softplus_small(-decay_logit[layer, way : way + 1])
            )
            decay = jnp.exp(log_a)
            drive = jnp.sqrt(neg_expm1(2.0 * log_a)) * gate(2 * way + 1) * conv32
            for lane in range(width // 128):
                coef[0, lane] = decay[:, lane * 128 : (lane + 1) * 128]
                coef[1, lane] = drive[:, lane * 128 : (lane + 1) * 128]
            prod = jnp.ones((8, width), F32)
            state = jnp.zeros((8, width), F32)
            for r in range(seg) if way == 0 else reversed(range(seg)):
                a, b = (
                    jnp.concatenate(
                        [coef[k, lane, pl.ds(r, 8, stride=seg), :] for lane in range(width // 128)],
                        axis=1,
                    )
                    for k in range(2)
                )
                state = a * state + b
                prod = a * prod
                local[way, 0, r] = prod
                local[way, 1, r] = state
            run_a = jnp.ones((1, width), F32)
            run_h = jnp.zeros((1, width), F32)
            heads = [None] * 8
            for s in range(8) if way == 0 else reversed(range(8)):
                heads[s] = (run_a, run_h)
                run_h = prod[s : s + 1] * run_h + state[s : s + 1]
                run_a = prod[s : s + 1] * run_a
            msg[layer, way, 0:1] = run_a
            msg[layer, way, 1:2] = run_h
            first.append(
                (
                    jnp.concatenate([h[0] for h in heads], axis=0),
                    jnp.concatenate([h[1] for h in heads], axis=0),
                )
            )

        def tell(d, _):
            remote(
                msg.at[layer, (p + d) // S],
                carries.at[layer, p],
                carry_sems.at[layer, 0],
                carry_sems.at[layer, 1],
                {"sp": lax.rem(p + d, S)},
            ).start()
            return 0

        lax.fori_loop(1, S, tell, 0)
        carries[layer, p] = msg[layer, 0]
        forward_some()
        bytes_of(carries.at[layer, pl.ds(0, S - 1)], carry_sems.at[layer, 1]).wait()

        def fold(j, held):
            ahead, behind = held
            one = carries[layer, j]
            ahead = jnp.where(j < p, one[0:1] * ahead + one[1:2], ahead)
            k = S - 1 - j
            one = carries[layer, k]
            behind = jnp.where(k > p, one[0:1] * behind + one[1:2], behind)
            return ahead, behind

        zero = jnp.zeros((1, width), F32)
        enter = lax.fori_loop(0, S, fold, (zero, zero), unroll=True)
        heads = [a * e + h for (a, h), e in zip(first, enter)]
        for r in range(seg):
            both = (
                local[0, 1, r]
                + local[0, 0, r] * heads[0]
                + local[1, 1, r]
                + local[1, 0, r] * heads[1]
            )
            for lane in range(width // 128):
                hidden[lane, pl.ds(r, 8, stride=seg), :] = both[:, lane * 128 : (lane + 1) * 128]
        states = jnp.concatenate([hidden[lane] for lane in range(width // 128)], axis=1)
        mix = (gated[...] * states).astype(BF16)
        block[layer] = mix
        across = spread[2 * layer + 1]
        acts[2 * layer + 1, t] = mix
        across.begin(block.at[layer])
        forward_some()
        across.wait()
        full = acts.at[2 * layer + 1]
        moved = jnp.zeros((rows, width), F32)
        for k in range(T):
            moved = moved + jnp.dot(full[k], weight(out_at, k), preferred_element_type=F32)
        before = tokens[...] if layer == 0 else block[2]
        resid = (before.astype(F32) + moved).astype(BF16)
        if layer < LAYERS - 1:
            block[2] = resid
            acts[2, t] = resid
            spread[2].begin(block.at[2])
            forward_some()
            spread[2].wait()

    wide = resid.astype(F32)
    own = jnp.sum(wide * wide, axis=1, keepdims=True)
    line = jnp.broadcast_to(own, (rows, rows)).T[0:1]
    squares[t] = line
    for d in range(1, T):
        copy = remote(
            squares.at[t], squares.at[t], square_sems.at[0], square_sems.at[1],
            {"tp": lax.rem(t + d, T)},
        )
        copy.start()
    bytes_of(squares.at[pl.ds(0, T - 1)], square_sems.at[1]).wait()
    total = squares[0]
    for k in range(1, T):
        total = total + squares[k]
    scale = lax.rsqrt(total / (T * width) + EPS)
    scale = jnp.broadcast_to(scale, (rows, rows)).T[:, 0:1]
    out[...] = (wide * scale * final_gain[...]).astype(BF16)

    for each in (ring_a, ring_b, ring_c, *spread):
        each.drain()
    for layer in range(LAYERS):
        bytes_of(carries.at[layer, pl.ds(0, S - 1)], carry_sems.at[layer, 0]).wait()
    bytes_of(squares.at[pl.ds(0, T - 1)], square_sems.at[0]).wait()


def body(S, T, *args):
    tokens, gate_maps, in_weight = args[0], args[6], args[2]
    args = (*args[:-1], args[-1][None])
    rows, width = tokens.shape
    depth = in_weight.shape[1]
    cols = gate_maps.shape[2]
    seg = rows // 8
    vmem = pl.BlockSpec(memory_space=pltpu.VMEM)
    dma = pltpu.SemaphoreType.DMA
    return pl.pallas_call(
        functools.partial(kernel, S, T),
        out_shape=jax.ShapeDtypeStruct((rows, width), BF16),
        in_specs=[vmem] * len(args),
        out_specs=vmem,
        scratch_shapes=[
            pltpu.VMEM((S, depth + cols, width), BF16),
            pltpu.VMEM((S, 2 * depth, width), BF16),
            pltpu.VMEM((S, 3 * depth + cols, width), BF16),
            pltpu.VMEM((4, T, rows, width), BF16),
            pltpu.VMEM((LAYERS, 2, 16, width), BF16),
            pltpu.VMEM((LAYERS, 2, 16, width), BF16),
            pltpu.VMEM((rows + 16, width), F32),
            pltpu.VMEM((2, width // 128, rows, 128), F32),
            pltpu.VMEM((2, 2, seg, 8, width), F32),
            pltpu.VMEM((width // 128, rows, 128), F32),
            pltpu.VMEM((rows, width), F32),
            pltpu.VMEM((LAYERS, 2, 2, width), F32),
            pltpu.VMEM((LAYERS, S, 2, width), F32),
            pltpu.VMEM((3, rows, width), BF16),
            pltpu.VMEM((T, 1, rows), F32),
            dma((3, 2, S // 4)),
            dma((3, 3)),
            dma((4, T - 1)),
            dma((4,)),
            dma((LAYERS, 4)),
            dma((LAYERS, 2)),
            dma((2,)),
        ],
        compiler_params=pltpu.CompilerParams(
            collective_id=0, has_side_effects=True, vmem_limit_bytes=40 * 2**20
        ),
        name="recurrent_layers",
    )(*args)


def solution(mesh):
    placed = (
        P(("grp", "sp"), "tp"),
        P(),
        P(None, "sp", "tp"),
        P(None, "sp", "tp"),
        P(None, None, "tp"),
        P(None, None, "tp"),
        P(None, "tp", "sp"),
        P(None, "sp", "tp"),
        P("tp"),
    )
    return jax.shard_map(
        functools.partial(body, mesh.shape["sp"], mesh.shape["tp"]),
        mesh=mesh,
        in_specs=placed,
        out_specs=P(("grp", "sp"), "tp"),
        check_vma=False,
    )
```

```python
import functools

import jax
import jax.numpy as jnp
from jax import lax
from jax.experimental import pallas as pl
from jax.experimental.pallas import tpu as pltpu
from jax.sharding import PartitionSpec as P

HEAD_W = 256
TAPS = 4
LAYERS = 2
EPS = 1e-06
F32 = jnp.float32
BF16 = jnp.bfloat16


def remote(src, dst, send, recv, where):
    return pltpu.make_async_remote_copy(
        src_ref=src,
        dst_ref=dst,
        send_sem=send,
        recv_sem=recv,
        device_id=where,
        device_id_type=pl.DeviceIdType.MESH,
    )


def bytes_of(ref, sem):
    return pltpu.make_async_copy(ref, ref, sem)


def softplus_small(x):
    y = jnp.exp(-jnp.abs(x))
    series = y * (1 - y * (1 / 2 - y * (1 / 3 - y * (1 / 4 - y * (1 / 5 - y * (1 / 6))))))
    return jnp.maximum(x, 0.0) + jnp.where(y < 0.05, series, jnp.log(1.0 + y))


def neg_expm1(x):
    tail = 1 + x * (1 / 6) * (1 + x * (1 / 7) * (1 + x * (1 / 8)))
    series = x * (1 + x * (1 / 2) * (1 + x * (1 / 3) * (1 + x * (1 / 4) * (1 + x * (1 / 5) * tail))))
    return -jnp.where(x > -0.5, series, jnp.exp(x) - 1.0)


class Gather:
    def __init__(self, held, sems, axis, size, place, reach, twins):
        self.held, self.axis, self.reach, self.twins = held, axis, reach, twins
        self.send, self.recv = sems[:2]
        self.size = size // 2 if twins else size
        self.half = self.size // 2
        self.own = place
        self.place = place // 2 if twins else place
        self.core = lax.rem(place, 2) if twins else None
        if twins:
            self.push_send, self.push_recv = sems[2:]
        self.rows = held.shape[1]
        self.stages = -(-self.half // reach)
        self.last = self.stages

    def slot(self, place):
        place = lax.rem(place + 2 * self.size, self.size)
        return place * 2 + self.core if self.twins else place

    def view(self, slot, flow, d):
        if d < self.half:
            return self.held.at[slot]
        rows = self.rows // 2
        return self.held.at[slot, pl.ds(flow * rows, rows)]

    def hop(self, flow, d, j):
        way = 1 - 2 * flow
        view = self.view(self.slot(self.place - way * (d - j)), flow, d)
        to = {self.axis: self.slot(self.place + way * j)}
        return remote(view, view, self.send, self.recv.at[flow, d - 1], to)

    def landed(self, flow, d):
        way = 1 - 2 * flow
        view = self.view(self.slot(self.place - way * d), flow, d)
        to = {self.axis: self.slot(self.place + way)}
        remote(view, view, self.send, self.recv.at[flow, d - 1], to).wait_recv()
        if self.twins and d < self.half:
            self.push(self.slot(self.place - way * d))

    def push(self, slot):
        view = self.held.at[slot]
        other = self.place * 2 + 1 - self.core
        remote(view, view, self.push_send, self.push_recv, {self.axis: other}).start()

    def emit(self, stage, flow):
        for j in range(self.reach, 0, -1):
            if self.reach * stage + j <= self.half:
                self.hop(flow, self.reach * stage + j, j).start()

    def begin(self):
        for flow in range(2):
            self.emit(0, flow)
        if self.twins:
            self.push(self.own)

    def step(self, stage):
        ahead = self.reach * stage
        if stage < self.stages:
            for flow in range(2):
                self.landed(flow, ahead)
                self.emit(stage, flow)
        for d in range(ahead - self.reach + 1, min(ahead, self.half) + 1):
            if stage < self.stages and d == ahead:
                continue
            for flow in range(2):
                self.landed(flow, d)
            if self.twins and d == self.half:
                self.push(self.slot(self.place + self.half))

    def wait(self, first=1):
        for stage in range(first, self.stages + 1):
            self.step(stage)

    def joined(self):
        bytes_of(self.held.at[pl.ds(0, self.size)], self.push_recv).wait()

    def drain(self):
        bytes_of(self.held.at[pl.ds(0, self.size - 1)], self.send).wait()
        if self.twins:
            bytes_of(self.held.at[pl.ds(0, self.size)], self.push_send).wait()


REACH_IN = 1
REACH_LATER = 1
REACH_X = 2


def kernel(
    S,
    T,
    tokens_hbm,
    norm_gain_hbm,
    in_weight,
    gate_weight,
    conv_taps_hbm,
    decay_logit_hbm,
    gate_maps,
    out_weight,
    final_gain_hbm,
    out,
    tokens,
    norm_gain,
    conv_taps,
    decay_logit,
    final_gain,
    held_in,
    held_map,
    held_gate,
    held_out,
    held_c,
    held_d,
    acts,
    normed,
    edges,
    edge_in,
    padded,
    coef,
    local,
    hidden,
    gated,
    msg,
    carries,
    block,
    squares,
    load_sems,
    ring_recv,
    ring_send,
    x_recv,
    x_send,
    edge_sems,
    carry_sems,
    square_sems,
):
    p = lax.axis_index("sp")
    t = lax.axis_index("tp")
    rows, width = tokens.shape
    depth = in_weight.shape[1]
    cols = gate_maps.shape[1]
    seg = rows // 8
    share = width // depth
    quarter = S // 4

    held = (held_in, held_map, held_gate, held_out, held_c, held_d)
    rings = [
        Gather(
            g,
            (ring_send.at[k, 0], ring_recv.at[k], ring_send.at[k, 1], ring_send.at[k, 2]),
            "sp",
            S,
            p,
            REACH_IN if k < 2 else REACH_LATER,
            True,
        )
        for k, g in enumerate(held)
    ]
    ring_in, ring_map, ring_gate, ring_out, ring_c, ring_d = rings
    spread = [
        Gather(acts.at[k], (x_send.at[k], x_recv.at[k]), "tp", T, t, REACH_X, False)
        for k in range(4)
    ]

    barrier = pltpu.get_barrier_semaphore()
    friends = [
        {"sp": ring_in.slot(ring_in.place + way * j)}
        for way in (1, -1)
        for j in range(1, REACH_IN + 1)
    ]
    friends.append({"sp": ring_in.place * 2 + 1 - ring_in.core})
    friends.extend({"tp": lax.rem(t + d, T)} for d in range(1, T))
    for friend in friends:
        pl.semaphore_signal(
            barrier, inc=1, device_id=friend, device_id_type=pl.DeviceIdType.MESH
        )

    loads = [
        (in_weight.at[0], held_in.at[p]),
        (gate_maps.at[0], held_map.at[p]),
        (tokens_hbm, tokens),
        (gate_weight.at[0], held_gate.at[p]),
        (out_weight.at[0], held_out.at[p]),
        (in_weight.at[1], held_c.at[p, pl.ds(0, depth)]),
        (gate_maps.at[1], held_c.at[p, pl.ds(depth, cols)]),
        (gate_weight.at[1], held_d.at[p, pl.ds(0, depth)]),
        (out_weight.at[1], held_d.at[p, pl.ds(depth, depth)]),
        (norm_gain_hbm, norm_gain),
        (conv_taps_hbm, conv_taps),
        (decay_logit_hbm, decay_logit),
        (final_gain_hbm, final_gain),
    ]
    loads = [
        pltpu.make_async_copy(src, dst, load_sems.at[k]) for k, (src, dst) in enumerate(loads)
    ]
    for load in loads:
        load.start()
    for load in loads:
        load.wait()
    acts[0, t] = tokens[...]
    with jax.named_scope("w_barrier"):
        pl.semaphore_wait(barrier, len(friends))

    ring_in.begin()
    ring_map.begin()
    spread[0].begin()

    def normalize(layer):
        full = acts.at[2 * layer]
        total = jnp.zeros((rows, 1), F32)
        for k in range(T):
            wide = full[k].astype(F32)
            total = total + jnp.sum(wide * wide, axis=1, keepdims=True)
        scale = lax.rsqrt(total / (T * width) + EPS)
        for k in range(T):
            wide = full[k].astype(F32)
            normed[k] = (
                wide * scale * norm_gain[layer : layer + 1, k * width : (k + 1) * width]
            ).astype(BF16)

    lagged = [ring_gate, ring_out]
    for step in range(1, ring_in.last + 1):
        with jax.named_scope("w_in%d" % step):
            ring_in.step(step)
            ring_map.step(step)
        with jax.named_scope("w_go%d" % step):
            for each in lagged:
                if step == 1:
                    each.begin()
                elif step <= each.last:
                    each.step(step - 1)
        if step == 1:
            with jax.named_scope("w_tok1"):
                spread[0].step(1)
        if step == max(1, ring_in.last - 1):
            with jax.named_scope("w_tokens"):
                spread[0].wait(2)
            normalize(0)
    with jax.named_scope("w_join"):
        ring_in.joined()

    def later(*steps):
        for step in steps:
            with jax.named_scope("w_c%d" % step):
                for each in (ring_c, ring_d):
                    if step == 0:
                        each.begin()
                    elif step <= each.last:
                        each.step(step)

    for layer in range(LAYERS):
        if layer == 0:
            in_at, map_at, gate_at, out_at = (held_in, 0), (held_map, 0), (held_gate, 0), (held_out, 0)
        else:
            in_at, map_at, gate_at, out_at = (held_c, 0), (held_c, depth), (held_d, 0), (held_d, depth)

        def weight(at, k):
            ref, row = at
            return ref[k * share : (k + 1) * share, row : row + depth].reshape(width, width)

        proj = jnp.zeros((rows, width), F32)
        for k in range(T):
            proj = proj + jnp.dot(normed[k], weight(in_at, k), preferred_element_type=F32)
        xin = proj.astype(BF16)
        edges[layer, 0] = xin[rows - 16 : rows]
        edges[layer, 1] = xin[0:16]
        up = remote(
            edges.at[layer, 0], edge_in.at[layer, 0], edge_sems.at[layer, 0], edge_sems.at[layer, 1],
            {"sp": lax.rem(p + 1, S)},
        )
        down = remote(
            edges.at[layer, 1], edge_in.at[layer, 1], edge_sems.at[layer, 2], edge_sems.at[layer, 3],
            {"sp": lax.rem(p + S - 1, S)},
        )
        up.start()
        down.start()
        padded[8 : 8 + rows] = xin.astype(F32)
        if layer == 0:
            with jax.named_scope("w_golast"):
                ring_map.joined()
                for each in lagged:
                    for step in range(min(ring_in.last, each.last), each.last + 1):
                        each.step(step)
            later(0)
        with jax.named_scope("w_halo"):
            up.wait()
            down.wait()
        before = edge_in[layer, 0].astype(F32)[8:16]
        after = edge_in[layer, 1].astype(F32)[0:8]
        padded[0:8] = jnp.where(p == 0, 0.0, before)
        padded[8 + rows : 16 + rows] = jnp.where(p == S - 1, 0.0, after)
        conv = conv_taps[layer, 0:1] * padded[6 : 6 + rows]
        for k in range(1, TAPS):
            conv = conv + conv_taps[layer, k : k + 1] * padded[6 + k : 6 + k + rows]
        conv = conv.astype(BF16)
        conv32 = conv.astype(F32)

        def gate(g):
            ref, row = map_at
            maps = ref[g * quarter : (g + 1) * quarter, row : row + cols].reshape(width, width)
            pre = lax.dot_general(
                conv, maps, (((1,), (1,)), ((), ())), preferred_element_type=F32
            )
            return jax.nn.sigmoid(pre)

        first = []
        for way in range(2):
            log_a = (
                -8.0 * gate(2 * way) * softplus_small(-decay_logit[layer, way : way + 1])
            )
            decay = jnp.exp(log_a)
            drive = jnp.sqrt(neg_expm1(2.0 * log_a)) * gate(2 * way + 1) * conv32
            for lane in range(width // 128):
                coef[0, lane] = decay[:, lane * 128 : (lane + 1) * 128]
                coef[1, lane] = drive[:, lane * 128 : (lane + 1) * 128]
            prod = jnp.ones((8, width), F32)
            state = jnp.zeros((8, width), F32)
            for r in range(seg) if way == 0 else reversed(range(seg)):
                a, b = (
                    jnp.concatenate(
                        [coef[k, lane, pl.ds(r, 8, stride=seg), :] for lane in range(width // 128)],
                        axis=1,
                    )
                    for k in range(2)
                )
                state = a * state + b
                prod = a * prod
                local[way, 0, r] = prod
                local[way, 1, r] = state
            run_a = jnp.ones((1, width), F32)
            run_h = jnp.zeros((1, width), F32)
            heads = [None] * 8
            for s in range(8) if way == 0 else reversed(range(8)):
                heads[s] = (run_a, run_h)
                run_h = prod[s : s + 1] * run_h + state[s : s + 1]
                run_a = prod[s : s + 1] * run_a
            msg[layer, way, 0:1] = run_a
            msg[layer, way, 1:2] = run_h
            first.append(
                (
                    jnp.concatenate([h[0] for h in heads], axis=0),
                    jnp.concatenate([h[1] for h in heads], axis=0),
                )
            )

        def tell(d, _):
            remote(
                msg.at[layer, (p + d) // S],
                carries.at[layer, p],
                carry_sems.at[layer, 0],
                carry_sems.at[layer, 1],
                {"sp": lax.rem(p + d, S)},
            ).start()
            return 0

        lax.fori_loop(1, S, tell, 0)
        carries[layer, p] = msg[layer, 0]
        if layer == 0:
            later(1)
            with jax.named_scope("w_joingate"):
                ring_gate.joined()
        else:
            with jax.named_scope("w_joind"):
                ring_d.joined()
        proj = jnp.zeros((rows, width), F32)
        for k in range(T):
            proj = proj + jnp.dot(normed[k], weight(gate_at, k), preferred_element_type=F32)
        gated[...] = jax.nn.gelu(proj.astype(BF16).astype(F32))
        if layer == 0:
            later(2, 3)
        with jax.named_scope("w_carry"):
            bytes_of(carries.at[layer, pl.ds(0, S - 1)], carry_sems.at[layer, 1]).wait()

        def fold(j, held):
            ahead, behind = held
            one = carries[layer, j]
            ahead = jnp.where(j < p, one[0:1] * ahead + one[1:2], ahead)
            k = S - 1 - j
            one = carries[layer, k]
            behind = jnp.where(k > p, one[0:1] * behind + one[1:2], behind)
            return ahead, behind

        zero = jnp.zeros((1, width), F32)
        enter = lax.fori_loop(0, S, fold, (zero, zero), unroll=True)
        heads = [a * e + h for (a, h), e in zip(first, enter)]
        for r in range(seg):
            both = (
                local[0, 1, r]
                + local[0, 0, r] * heads[0]
                + local[1, 1, r]
                + local[1, 0, r] * heads[1]
            )
            for lane in range(width // 128):
                hidden[lane, pl.ds(r, 8, stride=seg), :] = both[:, lane * 128 : (lane + 1) * 128]
        states = jnp.concatenate([hidden[lane] for lane in range(width // 128)], axis=1)
        mix = (gated[...] * states).astype(BF16)
        across = spread[2 * layer + 1]
        acts[2 * layer + 1, t] = mix
        across.begin()
        if layer == 0:
            later(4)
        with jax.named_scope("w_mix1"):
            across.step(1)
        if layer == 0:
            later(5, 6)
            with jax.named_scope("w_joinout"):
                ring_out.joined()
        with jax.named_scope("w_mix"):
            across.wait(2)
        full = acts.at[2 * layer + 1]
        moved = jnp.zeros((rows, width), F32)
        for k in range(T):
            moved = moved + jnp.dot(full[k], weight(out_at, k), preferred_element_type=F32)
        before = tokens[...] if layer == 0 else block[...]
        resid = (before.astype(F32) + moved).astype(BF16)
        if layer < LAYERS - 1:
            block[...] = resid
            acts[2, t] = resid
            spread[2].begin()
            later(7)
            with jax.named_scope("w_resid1"):
                spread[2].step(1)
            later(8)
            with jax.named_scope("w_joinc"):
                ring_c.joined()
            with jax.named_scope("w_resid"):
                spread[2].wait(2)
            normalize(1)

    wide = resid.astype(F32)
    own = jnp.sum(wide * wide, axis=1, keepdims=True)
    line = jnp.broadcast_to(own, (rows, rows)).T[0:1]
    squares[t] = line
    for d in range(1, T):
        copy = remote(
            squares.at[t], squares.at[t], square_sems.at[0], square_sems.at[1],
            {"tp": lax.rem(t + d, T)},
        )
        copy.start()
    with jax.named_scope("w_drain"):
        for each in (*rings, *spread):
            each.drain()
        for layer in range(LAYERS):
            bytes_of(carries.at[layer, pl.ds(0, S - 1)], carry_sems.at[layer, 0]).wait()
    with jax.named_scope("w_sq"):
        bytes_of(squares.at[pl.ds(0, T - 1)], square_sems.at[1]).wait()
    total = squares[0]
    for k in range(1, T):
        total = total + squares[k]
    scale = lax.rsqrt(total / (T * width) + EPS)
    scale = jnp.broadcast_to(scale, (rows, rows)).T[:, 0:1]
    out[...] = (wide * scale * final_gain[...]).astype(BF16)
    bytes_of(squares.at[pl.ds(0, T - 1)], square_sems.at[0]).wait()


def body(S, T, *args):
    tokens, gate_maps, in_weight = args[0], args[6], args[2]
    args = (*args[:6], jnp.swapaxes(gate_maps, 1, 2), args[7], args[8][None])
    rows, width = tokens.shape
    depth = in_weight.shape[1]
    cols = gate_maps.shape[2]
    seg = rows // 8
    dma = pltpu.SemaphoreType.DMA
    return pl.pallas_call(
        functools.partial(kernel, S, T),
        out_shape=jax.ShapeDtypeStruct((rows, width), BF16),
        in_specs=[pl.BlockSpec(memory_space=pltpu.HBM)] * len(args),
        out_specs=pl.BlockSpec(memory_space=pltpu.VMEM),
        scratch_shapes=[
            pltpu.VMEM((rows, width), BF16),
            pltpu.VMEM(args[1].shape, F32),
            pltpu.VMEM(args[4].shape, F32),
            pltpu.VMEM(args[5].shape, F32),
            pltpu.VMEM((1, width), F32),
            pltpu.VMEM((S, depth, width), BF16),
            pltpu.VMEM((S, cols, width), BF16),
            pltpu.VMEM((S, depth, width), BF16),
            pltpu.VMEM((S, depth, width), BF16),
            pltpu.VMEM((S, depth + cols, width), BF16),
            pltpu.VMEM((S, 2 * depth, width), BF16),
            pltpu.VMEM((4, T, rows, width), BF16),
            pltpu.VMEM((T, rows, width), BF16),
            pltpu.VMEM((LAYERS, 2, 16, width), BF16),
            pltpu.VMEM((LAYERS, 2, 16, width), BF16),
            pltpu.VMEM((rows + 16, width), F32),
            pltpu.VMEM((2, width // 128, rows, 128), F32),
            pltpu.VMEM((2, 2, seg, 8, width), F32),
            pltpu.VMEM((width // 128, rows, 128), F32),
            pltpu.VMEM((rows, width), F32),
            pltpu.VMEM((LAYERS, 2, 2, width), F32),
            pltpu.VMEM((LAYERS, S, 2, width), F32),
            pltpu.VMEM((rows, width), BF16),
            pltpu.VMEM((T, 1, rows), F32),
            dma((13,)),
            dma((6, 2, S // 4)),
            dma((6, 3)),
            dma((4, 2, T // 2)),
            dma((4,)),
            dma((LAYERS, 4)),
            dma((LAYERS, 2)),
            dma((2,)),
        ],
        compiler_params=pltpu.CompilerParams(
            collective_id=0, has_side_effects=True
        ),
        name="recurrent_layers",
    )(*args)


def solution(mesh):
    placed = (
        P(("grp", "sp"), "tp"),
        P(),
        P(None, "sp", "tp"),
        P(None, "sp", "tp"),
        P(None, None, "tp"),
        P(None, None, "tp"),
        P(None, "tp", "sp"),
        P(None, "sp", "tp"),
        P("tp"),
    )
    return jax.shard_map(
        functools.partial(body, mesh.shape["sp"], mesh.shape["tp"]),
        mesh=mesh,
        in_specs=placed,
        out_specs=P(("grp", "sp"), "tp"),
        check_vma=False,
    )
```

```python
import functools

import jax
import jax.numpy as jnp
from jax import lax
from jax.experimental import pallas as pl
from jax.experimental.pallas import tpu as pltpu
from jax.sharding import PartitionSpec as P

HEAD_W = 256
TAPS = 4
LAYERS = 2
EPS = 1e-06
F32 = jnp.float32
BF16 = jnp.bfloat16


def remote(src, dst, send, recv, where):
    return pltpu.make_async_remote_copy(
        src_ref=src,
        dst_ref=dst,
        send_sem=send,
        recv_sem=recv,
        device_id=where,
        device_id_type=pl.DeviceIdType.MESH,
    )


def bytes_of(ref, sem):
    return pltpu.make_async_copy(ref, ref, sem)


def softplus_small(x):
    y = jnp.exp(-jnp.abs(x))
    series = y * (1 - y * (1 / 2 - y * (1 / 3 - y * (1 / 4 - y * (1 / 5 - y * (1 / 6))))))
    return jnp.maximum(x, 0.0) + jnp.where(y < 0.05, series, jnp.log(1.0 + y))


def neg_expm1(x):
    tail = 1 + x * (1 / 6) * (1 + x * (1 / 7) * (1 + x * (1 / 8)))
    series = x * (1 + x * (1 / 2) * (1 + x * (1 / 3) * (1 + x * (1 / 4) * (1 + x * (1 / 5) * tail))))
    return -jnp.where(x > -0.5, series, jnp.exp(x) - 1.0)


class Gather:
    def __init__(self, held, sems, axis, size, place, reach, twins):
        self.held, self.axis, self.reach, self.twins = held, axis, reach, twins
        self.send, self.recv = sems[:2]
        self.size = size // 2 if twins else size
        self.half = self.size // 2
        self.own = place
        self.place = place // 2 if twins else place
        self.core = lax.rem(place, 2) if twins else None
        if twins:
            self.push_send, self.push_recv = sems[2:]
        self.rows = held.shape[1]
        self.stages = -(-self.half // reach)
        self.done = 0

    def slot(self, place):
        place = lax.rem(place + 2 * self.size, self.size)
        return place * 2 + self.core if self.twins else place

    def view(self, slot, flow, d):
        if d < self.half:
            return self.held.at[slot]
        rows = self.rows // 2
        return self.held.at[slot, pl.ds(flow * rows, rows)]

    def hop(self, flow, d, j):
        way = 1 - 2 * flow
        view = self.view(self.slot(self.place - way * (d - j)), flow, d)
        to = {self.axis: self.slot(self.place + way * j)}
        return remote(view, view, self.send, self.recv.at[flow, d - 1], to)

    def landed(self, flow, d):
        way = 1 - 2 * flow
        view = self.view(self.slot(self.place - way * d), flow, d)
        to = {self.axis: self.slot(self.place + way)}
        remote(view, view, self.send, self.recv.at[flow, d - 1], to).wait_recv()
        if self.twins and d < self.half:
            self.push(self.slot(self.place - way * d))

    def push(self, slot):
        view = self.held.at[slot]
        other = self.place * 2 + 1 - self.core
        remote(view, view, self.push_send, self.push_recv, {self.axis: other}).start()

    def emit(self, stage, flow):
        for j in range(self.reach, 0, -1):
            if self.reach * stage + j <= self.half:
                self.hop(flow, self.reach * stage + j, j).start()

    def begin(self):
        for flow in range(2):
            self.emit(0, flow)
        if self.twins:
            self.push(self.own)

    def step(self, stage):
        ahead = self.reach * stage
        if stage < self.stages:
            for flow in range(2):
                self.landed(flow, ahead)
                self.emit(stage, flow)
        for d in range(ahead - self.reach + 1, min(ahead, self.half) + 1):
            if stage < self.stages and d == ahead:
                continue
            for flow in range(2):
                self.landed(flow, d)
            if self.twins and d == self.half:
                self.push(self.slot(self.place + self.half))

    def wait(self, first=1):
        for stage in range(first, self.stages + 1):
            self.step(stage)

    def advance(self):
        if self.done == 0:
            self.begin()
        elif self.done <= self.stages:
            self.step(self.done)
        self.done += 1

    def joined(self):
        bytes_of(self.held.at[pl.ds(0, self.size)], self.push_recv).wait()

    def drain(self):
        bytes_of(self.held.at[pl.ds(0, self.size - 1)], self.send).wait()
        if self.twins:
            bytes_of(self.held.at[pl.ds(0, self.size)], self.push_send).wait()


REACH = (2, 2, 2, 2, 2, 2, 2)
REACH_X = 2
PARTS = 2
SLOTS = dict(
    a1="m", a2="mg", a3="mg", a4="mgo", x0="g", k0="oc", y0="o", p0="oc", q0="cd", r0="cd", s0="de", x1="de", y1="e", p1="e"
)


def kernel(
    S,
    T,
    tokens_hbm,
    norm_gain_hbm,
    in_weight,
    gate_weight,
    conv_taps_hbm,
    decay_logit_hbm,
    gate_maps,
    out_weight,
    final_gain_hbm,
    out,
    norm_gain,
    conv_taps,
    decay_logit,
    final_gain,
    held_in,
    held_map,
    held_gate,
    held_out,
    held_c,
    held_d,
    held_e,
    acts,
    normed,
    edges,
    edge_in,
    padded,
    coef,
    local,
    hidden,
    gated,
    msg,
    carries,
    block,
    squares,
    load_sems,
    ring_recv,
    ring_send,
    x_recv,
    x_send,
    edge_sems,
    carry_sems,
    square_sems,
):
    p = lax.axis_index("sp")
    t = lax.axis_index("tp")
    rows, width = acts.shape[2:]
    depth = in_weight.shape[1]
    cols = gate_maps.shape[1]
    seg = rows // 8
    share = width // depth
    quarter = S // 4

    held = (held_in, held_map, held_gate, held_out, held_c, held_d, held_e)
    rings = [
        Gather(
            g,
            (ring_send.at[k, 0], ring_recv.at[k], ring_send.at[k, 1], ring_send.at[k, 2]),
            "sp",
            S,
            p,
            REACH[k],
            True,
        )
        for k, g in enumerate(held)
    ]
    ring_in, ring_map, ring_gate, ring_out, ring_c, ring_d, ring_e = rings
    part = rows // PARTS
    spread = [
        [
            Gather(
                acts.at[k, :, pl.ds(h * part, part)],
                (x_send.at[k, h], x_recv.at[k, h]),
                "tp",
                T,
                t,
                REACH_X,
                False,
            )
            for h in range(PARTS)
        ]
        for k in range(4)
    ]

    def advance(*some):
        for each in some:
            with jax.named_scope("w_%d.%d" % (rings.index(each), each.done)):
                each.advance()

    def slot(name):
        for k in SLOTS.get(name, ""):
            advance(rings["imgocde".index(k)])

    def finish(each):
        with jax.named_scope("w_%d.f" % rings.index(each)):
            while each.done <= each.stages:
                each.advance()
            each.joined()

    barrier = pltpu.get_barrier_semaphore()
    friends = [
        {"sp": ring_in.slot(ring_in.place + way * j)}
        for way in (1, -1)
        for j in range(1, min(REACH[0], ring_in.half) + 1)
    ]
    friends.append({"sp": ring_in.place * 2 + 1 - ring_in.core})
    friends.extend({"tp": lax.rem(t + d, T)} for d in range(1, T))
    for friend in friends:
        pl.semaphore_signal(
            barrier, inc=1, device_id=friend, device_id_type=pl.DeviceIdType.MESH
        )

    loads = [
        (in_weight.at[0], held_in.at[p]),
        (gate_maps.at[0], held_map.at[p]),
        (tokens_hbm, acts.at[0, t]),
        (gate_weight.at[0], held_gate.at[p]),
        (out_weight.at[0], held_out.at[p]),
        (in_weight.at[1], held_c.at[p, pl.ds(0, depth)]),
        (gate_maps.at[1], held_c.at[p, pl.ds(depth, cols)]),
        (gate_weight.at[1], held_d.at[p]),
        (out_weight.at[1], held_e.at[p]),
        (norm_gain_hbm, norm_gain),
        (conv_taps_hbm, conv_taps),
        (decay_logit_hbm, decay_logit),
        (final_gain_hbm, final_gain),
    ]
    loads = [
        pltpu.make_async_copy(src, dst, load_sems.at[k]) for k, (src, dst) in enumerate(loads)
    ]
    for load in loads:
        load.start()
    for load in loads[:3]:
        load.wait()
    with jax.named_scope("w_barrier"):
        pl.semaphore_wait(barrier, len(friends))
    ring_in.begin()
    for each in spread[0]:
        each.begin()
    slot("a0")
    for load in loads[3:]:
        load.wait()

    def normalize(layer, h):
        piece = slice(h * part, (h + 1) * part)
        total = jnp.zeros((part, 1), F32)
        for k in range(T):
            wide = acts[2 * layer, k, piece].astype(F32)
            total = total + jnp.sum(wide * wide, axis=1, keepdims=True)
        scale = lax.rsqrt(total / (T * width) + EPS)
        for k in range(T):
            wide = acts[2 * layer, k, piece].astype(F32)
            normed[k, piece] = (
                wide * scale * norm_gain[layer : layer + 1, k * width : (k + 1) * width]
            ).astype(BF16)

    for step in range(1, ring_in.stages + 1):
        with jax.named_scope("w_in%d" % step):
            ring_in.step(step)
        if step == 1:
            with jax.named_scope("w_tok1"):
                for each in spread[0]:
                    each.step(1)
        slot("a%d" % step)
        if step == max(1, ring_in.stages - 1):
            with jax.named_scope("w_tokens"):
                for each in spread[0]:
                    each.wait(2)
            for h in range(PARTS):
                normalize(0, h)
    with jax.named_scope("w_join"):
        ring_in.joined()

    for layer in range(LAYERS):
        if layer == 0:
            in_at, map_at, gate_at, out_at = (held_in, 0), (held_map, 0), (held_gate, 0), (held_out, 0)
        else:
            in_at, map_at, gate_at, out_at = (held_c, 0), (held_c, depth), (held_d, 0), (held_e, 0)

        def weight(at, k):
            ref, row = at
            return ref[k * share : (k + 1) * share, row : row + depth].reshape(width, width)

        proj = jnp.zeros((rows, width), F32)
        for k in range(T):
            proj = proj + jnp.dot(normed[k], weight(in_at, k), preferred_element_type=F32)
        xin = proj.astype(BF16)
        edges[layer, 0] = xin[rows - 16 : rows]
        edges[layer, 1] = xin[0:16]
        up = remote(
            edges.at[layer, 0], edge_in.at[layer, 0], edge_sems.at[layer, 0], edge_sems.at[layer, 1],
            {"sp": lax.rem(p + 1, S)},
        )
        down = remote(
            edges.at[layer, 1], edge_in.at[layer, 1], edge_sems.at[layer, 2], edge_sems.at[layer, 3],
            {"sp": lax.rem(p + S - 1, S)},
        )
        up.start()
        down.start()
        padded[8 : 8 + rows] = xin.astype(F32)
        if layer == 0:
            slot("x0")
        else:
            slot("x1")
        with jax.named_scope("w_halo"):
            up.wait()
            down.wait()
        if layer == 0:
            finish(ring_map)
        before = edge_in[layer, 0].astype(F32)[8:16]
        after = edge_in[layer, 1].astype(F32)[0:8]
        padded[0:8] = jnp.where(p == 0, 0.0, before)
        padded[8 + rows : 16 + rows] = jnp.where(p == S - 1, 0.0, after)
        conv = conv_taps[layer, 0:1] * padded[6 : 6 + rows]
        for k in range(1, TAPS):
            conv = conv + conv_taps[layer, k : k + 1] * padded[6 + k : 6 + k + rows]
        conv = conv.astype(BF16)
        conv32 = conv.astype(F32)

        def gate(g):
            ref, row = map_at
            maps = ref[g * quarter : (g + 1) * quarter, row : row + cols].reshape(width, width)
            pre = lax.dot_general(
                conv, maps, (((1,), (1,)), ((), ())), preferred_element_type=F32
            )
            return jax.nn.sigmoid(pre)

        first = []
        for way in range(2):
            log_a = (
                -8.0 * gate(2 * way) * softplus_small(-decay_logit[layer, way : way + 1])
            )
            decay = jnp.exp(log_a)
            drive = jnp.sqrt(neg_expm1(2.0 * log_a)) * gate(2 * way + 1) * conv32
            for lane in range(width // 128):
                coef[0, lane] = decay[:, lane * 128 : (lane + 1) * 128]
                coef[1, lane] = drive[:, lane * 128 : (lane + 1) * 128]
            prod = jnp.ones((8, width), F32)
            state = jnp.zeros((8, width), F32)
            for r in range(seg) if way == 0 else reversed(range(seg)):
                a, b = (
                    jnp.concatenate(
                        [coef[k, lane, pl.ds(r, 8, stride=seg), :] for lane in range(width // 128)],
                        axis=1,
                    )
                    for k in range(2)
                )
                state = a * state + b
                prod = a * prod
                local[way, 0, r] = prod
                local[way, 1, r] = state
            run_a = jnp.ones((1, width), F32)
            run_h = jnp.zeros((1, width), F32)
            heads = [None] * 8
            for s in range(8) if way == 0 else reversed(range(8)):
                heads[s] = (run_a, run_h)
                run_h = prod[s : s + 1] * run_h + state[s : s + 1]
                run_a = prod[s : s + 1] * run_a
            msg[layer, way, 0:1] = run_a
            msg[layer, way, 1:2] = run_h
            first.append(
                (
                    jnp.concatenate([h[0] for h in heads], axis=0),
                    jnp.concatenate([h[1] for h in heads], axis=0),
                )
            )

        def tell(d, _):
            remote(
                msg.at[layer, (p + d) // S],
                carries.at[layer, p],
                carry_sems.at[layer, 0],
                carry_sems.at[layer, 1],
                {"sp": lax.rem(p + d, S)},
            ).start()
            return 0

        lax.fori_loop(1, S, tell, 0)
        carries[layer, p] = msg[layer, 0]
        if layer == 0:
            slot("k0")
            finish(ring_gate)
        else:
            slot("k1")
            finish(ring_d)
        proj = jnp.zeros((rows, width), F32)
        for k in range(T):
            proj = proj + jnp.dot(normed[k], weight(gate_at, k), preferred_element_type=F32)
        gated[...] = jax.nn.gelu(proj.astype(BF16).astype(F32))
        if layer == 0:
            slot("y0")
        else:
            slot("y1")
        with jax.named_scope("w_carry"):
            bytes_of(carries.at[layer, pl.ds(0, S - 1)], carry_sems.at[layer, 1]).wait()

        def fold(j, held):
            ahead, behind = held
            one = carries[layer, j]
            ahead = jnp.where(j < p, one[0:1] * ahead + one[1:2], ahead)
            k = S - 1 - j
            one = carries[layer, k]
            behind = jnp.where(k > p, one[0:1] * behind + one[1:2], behind)
            return ahead, behind

        zero = jnp.zeros((1, width), F32)
        enter = lax.fori_loop(0, S, fold, (zero, zero), unroll=True)
        heads = [a * e + h for (a, h), e in zip(first, enter)]
        for r in range(seg):
            both = (
                local[0, 1, r]
                + local[0, 0, r] * heads[0]
                + local[1, 1, r]
                + local[1, 0, r] * heads[1]
            )
            for lane in range(width // 128):
                hidden[lane, pl.ds(r, 8, stride=seg), :] = both[:, lane * 128 : (lane + 1) * 128]
        states = jnp.concatenate([hidden[lane] for lane in range(width // 128)], axis=1)
        mix = (gated[...] * states).astype(BF16)
        across = spread[2 * layer + 1]
        acts[2 * layer + 1, t] = mix
        for each in across:
            each.begin()
        slot("p%d" % layer)
        with jax.named_scope("w_mix1"):
            for each in across:
                each.step(1)
        if layer == 0:
            slot("q0")
            finish(ring_out)
        else:
            finish(ring_e)
        for h in range(PARTS):
            with jax.named_scope("w_mix"):
                across[h].wait(2)
            piece = slice(h * part, (h + 1) * part)
            moved = jnp.zeros((part, width), F32)
            for k in range(T):
                moved = moved + jnp.dot(
                    acts[2 * layer + 1, k, piece], weight(out_at, k), preferred_element_type=F32
                )
            resid = (acts[2 * layer, t, piece].astype(F32) + moved).astype(BF16)
            if layer < LAYERS - 1:
                acts[2, t, piece] = resid
                spread[2][h].begin()
            else:
                block[piece] = resid
        if layer < LAYERS - 1:
            slot("r0")
            with jax.named_scope("w_resid1"):
                for each in spread[2]:
                    each.step(1)
            slot("s0")
            for h in range(PARTS):
                with jax.named_scope("w_resid"):
                    spread[2][h].wait(2)
                normalize(1, h)
            finish(ring_c)

    resid = block[...]
    wide = resid.astype(F32)
    own = jnp.sum(wide * wide, axis=1, keepdims=True)
    line = jnp.broadcast_to(own, (rows, rows)).T[0:1]
    squares[t] = line
    for d in range(1, T):
        copy = remote(
            squares.at[t], squares.at[t], square_sems.at[0], square_sems.at[1],
            {"tp": lax.rem(t + d, T)},
        )
        copy.start()
    with jax.named_scope("w_drain"):
        for each in (*rings, *sum(spread, [])):
            each.drain()
        for layer in range(LAYERS):
            bytes_of(carries.at[layer, pl.ds(0, S - 1)], carry_sems.at[layer, 0]).wait()
    with jax.named_scope("w_sq"):
        bytes_of(squares.at[pl.ds(0, T - 1)], square_sems.at[1]).wait()
    total = squares[0]
    for k in range(1, T):
        total = total + squares[k]
    scale = lax.rsqrt(total / (T * width) + EPS)
    scale = jnp.broadcast_to(scale, (rows, rows)).T[:, 0:1]
    out[...] = (wide * scale * final_gain[...]).astype(BF16)
    bytes_of(squares.at[pl.ds(0, T - 1)], square_sems.at[0]).wait()


def body(S, T, *args):
    tokens, gate_maps, in_weight = args[0], args[6], args[2]
    args = (*args[:6], jnp.swapaxes(gate_maps, 1, 2), args[7], args[8][None])
    rows, width = tokens.shape
    depth = in_weight.shape[1]
    cols = gate_maps.shape[2]
    seg = rows // 8
    dma = pltpu.SemaphoreType.DMA
    return pl.pallas_call(
        functools.partial(kernel, S, T),
        out_shape=jax.ShapeDtypeStruct((rows, width), BF16),
        in_specs=[pl.BlockSpec(memory_space=pltpu.HBM)] * len(args),
        out_specs=pl.BlockSpec(memory_space=pltpu.VMEM),
        scratch_shapes=[
            pltpu.VMEM(args[1].shape, F32),
            pltpu.VMEM(args[4].shape, F32),
            pltpu.VMEM(args[5].shape, F32),
            pltpu.VMEM((1, width), F32),
            pltpu.VMEM((S, depth, width), BF16),
            pltpu.VMEM((S, cols, width), BF16),
            pltpu.VMEM((S, depth, width), BF16),
            pltpu.VMEM((S, depth, width), BF16),
            pltpu.VMEM((S, depth + cols, width), BF16),
            pltpu.VMEM((S, depth, width), BF16),
            pltpu.VMEM((S, depth, width), BF16),
            pltpu.VMEM((4, T, rows, width), BF16),
            pltpu.VMEM((T, rows, width), BF16),
            pltpu.VMEM((LAYERS, 2, 16, width), BF16),
            pltpu.VMEM((LAYERS, 2, 16, width), BF16),
            pltpu.VMEM((rows + 16, width), F32),
            pltpu.VMEM((2, width // 128, rows, 128), F32),
            pltpu.VMEM((2, 2, seg, 8, width), F32),
            pltpu.VMEM((width // 128, rows, 128), F32),
            pltpu.VMEM((rows, width), F32),
            pltpu.VMEM((LAYERS, 2, 2, width), F32),
            pltpu.VMEM((LAYERS, S, 2, width), F32),
            pltpu.VMEM((rows, width), BF16),
            pltpu.VMEM((T, 1, rows), F32),
            dma((13,)),
            dma((7, 2, S // 4)),
            dma((7, 3)),
            dma((4, PARTS, 2, T // 2)),
            dma((4, PARTS)),
            dma((LAYERS, 4)),
            dma((LAYERS, 2)),
            dma((2,)),
        ],
        compiler_params=pltpu.CompilerParams(
            collective_id=0, has_side_effects=True
        ),
        name="recurrent_layers",
    )(*args)


def solution(mesh):
    placed = (
        P(("grp", "sp"), "tp"),
        P(),
        P(None, "sp", "tp"),
        P(None, "sp", "tp"),
        P(None, None, "tp"),
        P(None, None, "tp"),
        P(None, "tp", "sp"),
        P(None, "sp", "tp"),
        P("tp"),
    )
    return jax.shard_map(
        functools.partial(body, mesh.shape["sp"], mesh.shape["tp"]),
        mesh=mesh,
        in_specs=placed,
        out_specs=P(("grp", "sp"), "tp"),
        check_vma=False,
    )
```

```python
import functools

import jax
import jax.numpy as jnp
from jax import lax
from jax.experimental import pallas as pl
from jax.experimental.pallas import tpu as pltpu
from jax.sharding import PartitionSpec as P

HEAD_W = 256
TAPS = 4
LAYERS = 2
EPS = 1e-06
F32 = jnp.float32
BF16 = jnp.bfloat16


def remote(src, dst, send, recv, where):
    return pltpu.make_async_remote_copy(
        src_ref=src,
        dst_ref=dst,
        send_sem=send,
        recv_sem=recv,
        device_id=where,
        device_id_type=pl.DeviceIdType.MESH,
    )


def bytes_of(ref, sem):
    return pltpu.make_async_copy(ref, ref, sem)


def softplus_small(x):
    y = jnp.exp(-jnp.abs(x))
    series = y * (1 - y * (1 / 2 - y * (1 / 3 - y * (1 / 4 - y * (1 / 5 - y * (1 / 6))))))
    return jnp.maximum(x, 0.0) + jnp.where(y < 0.05, series, jnp.log(1.0 + y))


def neg_expm1(x, half):
    tail = 1 + x * (1 / 6) * (1 + x * (1 / 7) * (1 + x * (1 / 8)))
    series = x * (1 + x * (1 / 2) * (1 + x * (1 / 3) * (1 + x * (1 / 4) * (1 + x * (1 / 5) * tail))))
    return jnp.where(x > -0.5, -series, 1.0 - half * half)


class Gather:
    def __init__(self, held, sems, axis, size, place, reach, twins):
        self.held, self.axis, self.reach, self.twins = held, axis, reach, twins
        self.send, self.recv = sems[:2]
        self.size = size // 2 if twins else size
        self.half = self.size // 2
        self.own = place
        self.place = place // 2 if twins else place
        self.core = lax.rem(place, 2) if twins else None
        if twins:
            self.push_send, self.push_recv = sems[2:]
        self.rows = held.shape[1]
        self.stages = -(-self.half // reach)
        self.done = 0

    def slot(self, place):
        place = lax.rem(place + 2 * self.size, self.size)
        return place * 2 + self.core if self.twins else place

    def view(self, slot, flow, d):
        if d < self.half:
            return self.held.at[slot]
        rows = self.rows // 2
        return self.held.at[slot, pl.ds(flow * rows, rows)]

    def hop(self, flow, d, j):
        way = 1 - 2 * flow
        view = self.view(self.slot(self.place - way * (d - j)), flow, d)
        to = {self.axis: self.slot(self.place + way * j)}
        return remote(view, view, self.send, self.recv.at[flow, d - 1], to)

    def landed(self, flow, d):
        way = 1 - 2 * flow
        view = self.view(self.slot(self.place - way * d), flow, d)
        to = {self.axis: self.slot(self.place + way)}
        remote(view, view, self.send, self.recv.at[flow, d - 1], to).wait_recv()
        if self.twins and d < self.half:
            self.push(self.slot(self.place - way * d))

    def push(self, slot):
        view = self.held.at[slot]
        other = self.place * 2 + 1 - self.core
        remote(view, view, self.push_send, self.push_recv, {self.axis: other}).start()

    def emit(self, stage, flow):
        for j in range(self.reach, 0, -1):
            if self.reach * stage + j <= self.half:
                self.hop(flow, self.reach * stage + j, j).start()

    def begin(self):
        for flow in range(2):
            self.emit(0, flow)
        if self.twins:
            self.push(self.own)

    def step(self, stage):
        ahead = self.reach * stage
        if stage < self.stages:
            for flow in range(2):
                self.landed(flow, ahead)
                self.emit(stage, flow)
        for d in range(ahead - self.reach + 1, min(ahead, self.half) + 1):
            if stage < self.stages and d == ahead:
                continue
            for flow in range(2):
                self.landed(flow, d)
            if self.twins and d == self.half:
                self.push(self.slot(self.place + self.half))

    def wait(self, first=1):
        for stage in range(first, self.stages + 1):
            self.step(stage)

    def advance(self):
        if self.done == 0:
            self.begin()
        elif self.done <= self.stages:
            self.step(self.done)
        self.done += 1

    def joined(self):
        bytes_of(self.held.at[pl.ds(0, self.size)], self.push_recv).wait()

    def drain(self):
        bytes_of(self.held.at[pl.ds(0, self.size - 1)], self.send).wait()
        if self.twins:
            bytes_of(self.held.at[pl.ds(0, self.size)], self.push_send).wait()


REACH = (2, 2, 2, 2, 2, 2, 2)
REACH_X = 2
PARTS = 2
SLOTS = dict(
    a1="m", a2="mg", a3="mg", a4="mgo", x0="g", k0="oc", y0="o", p0="oc", q0="cd", r0="cd", s0="de", x1="de", y1="e", p1="e"
)


def kernel(
    S,
    T,
    tokens_hbm,
    norm_gain_hbm,
    in_weight,
    gate_weight,
    conv_taps_hbm,
    decay_logit_hbm,
    gate_maps,
    out_weight,
    final_gain_hbm,
    out,
    norm_gain,
    conv_taps,
    decay_logit,
    final_gain,
    held_in,
    held_map,
    held_gate,
    held_out,
    held_c,
    held_d,
    held_e,
    acts,
    normed,
    edges,
    edge_in,
    padded,
    coef,
    local,
    hidden,
    gated,
    msg,
    carries,
    block,
    squares,
    load_sems,
    ring_recv,
    ring_send,
    x_recv,
    x_send,
    edge_sems,
    carry_sems,
    square_sems,
):
    p = lax.axis_index("sp")
    t = lax.axis_index("tp")
    rows, width = acts.shape[2:]
    depth = in_weight.shape[1]
    cols = gate_maps.shape[1]
    seg = rows // 8
    share = width // depth
    quarter = S // 4

    held = (held_in, held_map, held_gate, held_out, held_c, held_d, held_e)
    rings = [
        Gather(
            g,
            (ring_send.at[k, 0], ring_recv.at[k], ring_send.at[k, 1], ring_send.at[k, 2]),
            "sp",
            S,
            p,
            REACH[k],
            True,
        )
        for k, g in enumerate(held)
    ]
    ring_in, ring_map, ring_gate, ring_out, ring_c, ring_d, ring_e = rings
    part = rows // PARTS
    spread = [
        [
            Gather(
                acts.at[k, :, pl.ds(h * part, part)],
                (x_send.at[k, h], x_recv.at[k, h]),
                "tp",
                T,
                t,
                REACH_X,
                False,
            )
            for h in range(PARTS)
        ]
        for k in range(4)
    ]

    def advance(*some):
        for each in some:
            with jax.named_scope("w_%d.%d" % (rings.index(each), each.done)):
                each.advance()

    def slot(name):
        for k in SLOTS.get(name, ""):
            advance(rings["imgocde".index(k)])

    def finish(each):
        with jax.named_scope("w_%d.f" % rings.index(each)):
            while each.done <= each.stages:
                each.advance()
            each.joined()

    barrier = pltpu.get_barrier_semaphore()
    friends = [
        {"sp": ring_in.slot(ring_in.place + way * j)}
        for way in (1, -1)
        for j in range(1, min(REACH[0], ring_in.half) + 1)
    ]
    friends.append({"sp": ring_in.place * 2 + 1 - ring_in.core})
    friends.extend({"tp": lax.rem(t + d, T)} for d in range(1, T))
    for friend in friends:
        pl.semaphore_signal(
            barrier, inc=1, device_id=friend, device_id_type=pl.DeviceIdType.MESH
        )

    loads = [
        (in_weight.at[0], held_in.at[p]),
        (gate_maps.at[0], held_map.at[p]),
        (tokens_hbm, acts.at[0, t]),
        (gate_weight.at[0], held_gate.at[p]),
        (out_weight.at[0], held_out.at[p]),
        (in_weight.at[1], held_c.at[p, pl.ds(0, depth)]),
        (gate_maps.at[1], held_c.at[p, pl.ds(depth, cols)]),
        (gate_weight.at[1], held_d.at[p]),
        (out_weight.at[1], held_e.at[p]),
        (norm_gain_hbm, norm_gain),
        (conv_taps_hbm, conv_taps),
        (decay_logit_hbm, decay_logit),
        (final_gain_hbm, final_gain),
    ]
    loads = [
        pltpu.make_async_copy(src, dst, load_sems.at[k]) for k, (src, dst) in enumerate(loads)
    ]
    for load in loads:
        load.start()
    for load in loads[:3]:
        load.wait()
    with jax.named_scope("w_barrier"):
        pl.semaphore_wait(barrier, len(friends))
    ring_in.begin()
    for each in spread[0]:
        each.begin()
    slot("a0")
    for load in loads[3:]:
        load.wait()

    def normalize(layer, h):
        piece = slice(h * part, (h + 1) * part)
        total = jnp.zeros((part, 1), F32)
        for k in range(T):
            wide = acts[2 * layer, k, piece].astype(F32)
            total = total + jnp.sum(wide * wide, axis=1, keepdims=True)
        scale = lax.rsqrt(total / (T * width) + EPS)
        for k in range(T):
            wide = acts[2 * layer, k, piece].astype(F32)
            normed[k, piece] = (
                wide * scale * norm_gain[layer : layer + 1, k * width : (k + 1) * width]
            ).astype(BF16)

    for step in range(1, ring_in.stages + 1):
        with jax.named_scope("w_in%d" % step):
            ring_in.step(step)
        if step == 1:
            with jax.named_scope("w_tok1"):
                for each in spread[0]:
                    each.step(1)
        slot("a%d" % step)
        if step == max(1, ring_in.stages - 1):
            with jax.named_scope("w_tokens"):
                for each in spread[0]:
                    each.wait(2)
            for h in range(PARTS):
                normalize(0, h)
    with jax.named_scope("w_join"):
        ring_in.joined()

    for layer in range(LAYERS):
        if layer == 0:
            in_at, map_at, gate_at, out_at = (held_in, 0), (held_map, 0), (held_gate, 0), (held_out, 0)
        else:
            in_at, map_at, gate_at, out_at = (held_c, 0), (held_c, depth), (held_d, 0), (held_e, 0)

        def weight(at, k):
            ref, row = at
            return ref[k * share : (k + 1) * share, row : row + depth].reshape(width, width)

        proj = jnp.zeros((rows, width), F32)
        for k in range(T):
            proj = proj + jnp.dot(normed[k], weight(in_at, k), preferred_element_type=F32)
        xin = proj.astype(BF16)
        edges[layer, 0] = xin[rows - 16 : rows]
        edges[layer, 1] = xin[0:16]
        up = remote(
            edges.at[layer, 0], edge_in.at[layer, 0], edge_sems.at[layer, 0], edge_sems.at[layer, 1],
            {"sp": lax.rem(p + 1, S)},
        )
        down = remote(
            edges.at[layer, 1], edge_in.at[layer, 1], edge_sems.at[layer, 2], edge_sems.at[layer, 3],
            {"sp": lax.rem(p + S - 1, S)},
        )
        up.start()
        down.start()
        padded[8 : 8 + rows] = xin.astype(F32)
        if layer == 0:
            slot("x0")
        else:
            slot("x1")
        with jax.named_scope("w_halo"):
            up.wait()
            down.wait()
        if layer == 0:
            finish(ring_map)
        before = edge_in[layer, 0].astype(F32)[8:16]
        after = edge_in[layer, 1].astype(F32)[0:8]
        padded[0:8] = jnp.where(p == 0, 0.0, before)
        padded[8 + rows : 16 + rows] = jnp.where(p == S - 1, 0.0, after)
        conv = conv_taps[layer, 0:1] * padded[6 : 6 + rows]
        for k in range(1, TAPS):
            conv = conv + conv_taps[layer, k : k + 1] * padded[6 + k : 6 + k + rows]
        conv = conv.astype(BF16)
        conv32 = conv.astype(F32)

        def gate(g):
            ref, row = map_at
            maps = ref[g * quarter : (g + 1) * quarter, row : row + cols].reshape(width, width)
            pre = lax.dot_general(
                conv, maps, (((1,), (1,)), ((), ())), preferred_element_type=F32
            )
            return jax.nn.sigmoid(pre)

        first = []
        for way in range(2):
            log_a = (
                -8.0 * gate(2 * way) * softplus_small(-decay_logit[layer, way : way + 1])
            )
            decay = jnp.exp(log_a)
            drive = jnp.sqrt(neg_expm1(2.0 * log_a, decay)) * gate(2 * way + 1) * conv32
            for lane in range(width // 128):
                coef[0, lane] = decay[:, lane * 128 : (lane + 1) * 128]
                coef[1, lane] = drive[:, lane * 128 : (lane + 1) * 128]
            prod = jnp.ones((8, width), F32)
            state = jnp.zeros((8, width), F32)
            for r in range(seg) if way == 0 else reversed(range(seg)):
                a, b = (
                    jnp.concatenate(
                        [coef[k, lane, pl.ds(r, 8, stride=seg), :] for lane in range(width // 128)],
                        axis=1,
                    )
                    for k in range(2)
                )
                state = a * state + b
                prod = a * prod
                local[way, 0, r] = prod
                local[way, 1, r] = state
            run_a = jnp.ones((1, width), F32)
            run_h = jnp.zeros((1, width), F32)
            heads = [None] * 8
            for s in range(8) if way == 0 else reversed(range(8)):
                heads[s] = (run_a, run_h)
                run_h = prod[s : s + 1] * run_h + state[s : s + 1]
                run_a = prod[s : s + 1] * run_a
            msg[layer, way, 0:1] = run_a
            msg[layer, way, 1:2] = run_h
            first.append(
                (
                    jnp.concatenate([h[0] for h in heads], axis=0),
                    jnp.concatenate([h[1] for h in heads], axis=0),
                )
            )

        def tell(d, _):
            remote(
                msg.at[layer, (p + d) // S],
                carries.at[layer, p],
                carry_sems.at[layer, 0],
                carry_sems.at[layer, 1],
                {"sp": lax.rem(p + d, S)},
            ).start()
            return 0

        lax.fori_loop(1, S, tell, 0)
        carries[layer, p] = msg[layer, 0]
        if layer == 0:
            slot("k0")
            finish(ring_gate)
        else:
            slot("k1")
            finish(ring_d)
        proj = jnp.zeros((rows, width), F32)
        for k in range(T):
            proj = proj + jnp.dot(normed[k], weight(gate_at, k), preferred_element_type=F32)
        gated[...] = jax.nn.gelu(proj.astype(BF16).astype(F32))
        if layer == 0:
            slot("y0")
        else:
            slot("y1")
        with jax.named_scope("w_carry"):
            bytes_of(carries.at[layer, pl.ds(0, S - 1)], carry_sems.at[layer, 1]).wait()

        def fold(j, held):
            ahead, behind = held
            one = carries[layer, j]
            ahead = jnp.where(j < p, one[0:1] * ahead + one[1:2], ahead)
            k = S - 1 - j
            one = carries[layer, k]
            behind = jnp.where(k > p, one[0:1] * behind + one[1:2], behind)
            return ahead, behind

        zero = jnp.zeros((1, width), F32)
        enter = lax.fori_loop(0, S, fold, (zero, zero), unroll=True)
        heads = [a * e + h for (a, h), e in zip(first, enter)]
        for r in range(seg):
            both = (
                local[0, 1, r]
                + local[0, 0, r] * heads[0]
                + local[1, 1, r]
                + local[1, 0, r] * heads[1]
            )
            for lane in range(width // 128):
                hidden[lane, pl.ds(r, 8, stride=seg), :] = both[:, lane * 128 : (lane + 1) * 128]
        states = jnp.concatenate([hidden[lane] for lane in range(width // 128)], axis=1)
        mix = (gated[...] * states).astype(BF16)
        across = spread[2 * layer + 1]
        acts[2 * layer + 1, t] = mix
        for each in across:
            each.begin()
        slot("p%d" % layer)
        with jax.named_scope("w_mix1"):
            for each in across:
                each.step(1)
        if layer == 0:
            slot("q0")
            finish(ring_out)
        else:
            finish(ring_e)
        for h in range(PARTS):
            with jax.named_scope("w_mix"):
                across[h].wait(2)
            piece = slice(h * part, (h + 1) * part)
            moved = jnp.zeros((part, width), F32)
            for k in range(T):
                moved = moved + jnp.dot(
                    acts[2 * layer + 1, k, piece], weight(out_at, k), preferred_element_type=F32
                )
            resid = (acts[2 * layer, t, piece].astype(F32) + moved).astype(BF16)
            if layer < LAYERS - 1:
                acts[2, t, piece] = resid
                spread[2][h].begin()
            else:
                block[piece] = resid
        if layer < LAYERS - 1:
            slot("r0")
            with jax.named_scope("w_resid1"):
                for each in spread[2]:
                    each.step(1)
            slot("s0")
            for h in range(PARTS):
                with jax.named_scope("w_resid"):
                    spread[2][h].wait(2)
                normalize(1, h)
            finish(ring_c)

    resid = block[...]
    wide = resid.astype(F32)
    own = jnp.sum(wide * wide, axis=1, keepdims=True)
    line = jnp.broadcast_to(own, (rows, rows)).T[0:1]
    squares[t] = line
    weighed = wide * final_gain[...]
    for d in range(1, T):
        copy = remote(
            squares.at[t], squares.at[t], square_sems.at[0], square_sems.at[1],
            {"tp": lax.rem(t + d, T)},
        )
        copy.start()
    with jax.named_scope("w_drain"):
        for each in (*rings, *sum(spread, [])):
            each.drain()
        for layer in range(LAYERS):
            bytes_of(carries.at[layer, pl.ds(0, S - 1)], carry_sems.at[layer, 0]).wait()
    with jax.named_scope("w_sq"):
        bytes_of(squares.at[pl.ds(0, T - 1)], square_sems.at[1]).wait()
    total = squares[0]
    for k in range(1, T):
        total = total + squares[k]
    scale = lax.rsqrt(total / (T * width) + EPS)
    scale = jnp.broadcast_to(scale, (rows, rows)).T[:, 0:1]
    out[...] = (weighed * scale).astype(BF16)
    bytes_of(squares.at[pl.ds(0, T - 1)], square_sems.at[0]).wait()


def body(S, T, *args):
    tokens, gate_maps, in_weight = args[0], args[6], args[2]
    args = (*args[:6], jnp.swapaxes(gate_maps, 1, 2), args[7], args[8][None])
    rows, width = tokens.shape
    depth = in_weight.shape[1]
    cols = gate_maps.shape[2]
    seg = rows // 8
    dma = pltpu.SemaphoreType.DMA
    return pl.pallas_call(
        functools.partial(kernel, S, T),
        out_shape=jax.ShapeDtypeStruct((rows, width), BF16),
        in_specs=[pl.BlockSpec(memory_space=pltpu.HBM)] * len(args),
        out_specs=pl.BlockSpec(memory_space=pltpu.VMEM),
        scratch_shapes=[
            pltpu.VMEM(args[1].shape, F32),
            pltpu.VMEM(args[4].shape, F32),
            pltpu.VMEM(args[5].shape, F32),
            pltpu.VMEM((1, width), F32),
            pltpu.VMEM((S, depth, width), BF16),
            pltpu.VMEM((S, cols, width), BF16),
            pltpu.VMEM((S, depth, width), BF16),
            pltpu.VMEM((S, depth, width), BF16),
            pltpu.VMEM((S, depth + cols, width), BF16),
            pltpu.VMEM((S, depth, width), BF16),
            pltpu.VMEM((S, depth, width), BF16),
            pltpu.VMEM((4, T, rows, width), BF16),
            pltpu.VMEM((T, rows, width), BF16),
            pltpu.VMEM((LAYERS, 2, 16, width), BF16),
            pltpu.VMEM((LAYERS, 2, 16, width), BF16),
            pltpu.VMEM((rows + 16, width), F32),
            pltpu.VMEM((2, width // 128, rows, 128), F32),
            pltpu.VMEM((2, 2, seg, 8, width), F32),
            pltpu.VMEM((width // 128, rows, 128), F32),
            pltpu.VMEM((rows, width), F32),
            pltpu.VMEM((LAYERS, 2, 2, width), F32),
            pltpu.VMEM((LAYERS, S, 2, width), F32),
            pltpu.VMEM((rows, width), BF16),
            pltpu.VMEM((T, 1, rows), F32),
            dma((13,)),
            dma((7, 2, S // 4)),
            dma((7, 3)),
            dma((4, PARTS, 2, T // 2)),
            dma((4, PARTS)),
            dma((LAYERS, 4)),
            dma((LAYERS, 2)),
            dma((2,)),
        ],
        compiler_params=pltpu.CompilerParams(
            collective_id=0, has_side_effects=True
        ),
        name="recurrent_layers",
    )(*args)


def solution(mesh):
    placed = (
        P(("grp", "sp"), "tp"),
        P(),
        P(None, "sp", "tp"),
        P(None, "sp", "tp"),
        P(None, None, "tp"),
        P(None, None, "tp"),
        P(None, "tp", "sp"),
        P(None, "sp", "tp"),
        P("tp"),
    )
    return jax.shard_map(
        functools.partial(body, mesh.shape["sp"], mesh.shape["tp"]),
        mesh=mesh,
        in_specs=placed,
        out_specs=P(("grp", "sp"), "tp"),
        check_vma=False,
    )
```
